512 devices in a mesh: rep: 2 (over z_hi), fs: 32 (over z_lo, y), tp: 8 (over x, core).
Axes of the slice: x: 4, y: 8, z: 8 (z_hi: 2, z_lo: 4; z = z_hi * 4 + z_lo), core: 2. Of those that a mesh axis runs over, the one named last changes fastest.
Arguments:
- tokens: bfloat16 [65536, 1536], P(('rep', 'fs', 'tp')), may hold values from -6 to 6
- norm_gain: float32 [1536], replicated, may hold values from 0.1 to 1.9
- up_weight: float32 [1536, 6144], P('fs', 'tp'), may hold values from -0.15625 to 0.15625
- up_scale: float32 [1, 6144], P(None, 'tp'), may hold values from 0.5 to 2
- down_weight: float32 [6144, 1536], P('tp', 'fs'), may hold values from -0.078125 to 0.078125
- down_scale: float32 [1, 1536], P(None, 'fs'), may hold values from 0.5 to 2
Outputs:
- mixed: bfloat16 [65536, 1536], P(('rep', 'fs', 'tp'))
The draws below stay inside these ranges and needn't reach their ends.
All inputs are finite; a program needn't handle non-finite values.
Results may differ from the reference program's by a relative error of at most 0.015.
Values may be sent and summed in bfloat16 or wider, within the bound.
No kernel may reach another device: no remote copies, remote signals or barrier semaphores. Data moves between devices by JAX's collectives and lax.ppermute only.
A program may use at most 64 MiB of HBM per device.

```python
import math
import jax
import jax.numpy as jnp
from jax import lax

D = 1536
FF = 6144
TOK_DEV = 128
TOKENS = 65536
N_TP = 8


def steps_of(rng, extent, pieces, smallest, top_value):
    factor_of, own = 1.0, jax.random.fold_in(rng, 6)
    for dim, parts in pieces:
        steps = jnp.exp(jax.random.uniform(jax.random.fold_in(own, dim), (parts,), jnp.float32, smallest / len(pieces), top_value / len(pieces)))
        factor_of = factor_of * jnp.repeat(steps, extent[dim] // parts).reshape([-1 if axis == dim else 1 for axis in range(len(extent))])
    return factor_of


def noise(stream_key, shape, deviation, most, shards=(), dtype=jnp.bfloat16):
    drawn = jax.random.normal(stream_key, shape, jnp.float32) * deviation
    if len(shards) > 0:
        drawn = steps_of(stream_key, shape, shards, -0.22, 0.18) * drawn
    return jnp.clip(drawn, min=-most, max=most).astype(dtype)


def setup_inputs(seed: int = 0) -> dict:
    key_list = jax.random.split(jax.random.key(seed), 7)
    return {
        "tokens": noise(key_list[0], (TOKENS, D), 1.0, 6.0, ((0, 512),)),
        "norm_gain": jnp.clip(1.0 + 0.18 * jax.random.normal(key_list[1], (D,), jnp.float32), 0.1, 1.9),
        "up_weight": noise(key_list[2], (D, FF), D ** -0.5, 0.15625, ((0, 32), (1, 8)), jnp.float32),
        "up_scale": jnp.clip(jnp.exp(math.log(2.0) - 1.3862944 * jax.random.uniform(key_list[3], (1, FF), jnp.float32) ** steps_of(key_list[3], (1, FF), ((1, 8),), -0.2, 0.2)), 0.5, 2.0),
        "down_weight": noise(key_list[4], (FF, D), FF ** -0.5, 0.078125, ((0, 8), (1, 32)), jnp.float32),
        "down_scale": jnp.clip(jnp.exp(math.log(2.0) - 1.3862944 * jax.random.uniform(key_list[5], (1, D), jnp.float32) ** steps_of(key_list[5], (1, D), ((1, 32),), -0.2, 0.2)), 0.5, 2.0),
    }


def reference(tokens, norm_gain, up_weight, up_scale, down_weight, down_scale):
    up_cast = up_weight.astype(jnp.bfloat16)
    down_cast = down_weight.astype(jnp.bfloat16)
    width = FF // N_TP
    down_blocks = down_cast.reshape(N_TP, width, D).astype(jnp.float32)
    group_rows = TOK_DEV * N_TP
    groups = tokens.reshape(TOKENS // group_rows, group_rows, D)

    def one_group(rows):
        values = rows.astype(jnp.float32)
        normed = (values * lax.rsqrt(lax.optimization_barrier(jnp.mean(values * values, axis=-1, keepdims=True)) + 1e-06) * norm_gain).astype(jnp.bfloat16)
        pre = jnp.dot(normed, up_cast, preferred_element_type=jnp.float32) * up_scale
        hidden = jnp.square(jnp.maximum(pre, 0.0)).astype(jnp.bfloat16)
        hidden_blocks = hidden.reshape(group_rows, N_TP, width).astype(jnp.float32)
        partial_value = jnp.einsum('rkf,kfd->krd', hidden_blocks, down_blocks) * down_scale
        partial_value = partial_value.astype(jnp.bfloat16).astype(jnp.float32)
        return lax.optimization_barrier(jnp.sum(partial_value, axis=0)).astype(jnp.bfloat16)
    return lax.map(one_group, groups).reshape(TOKENS, D)
```

```python
import jax
import jax.numpy as jnp
from jax import lax
from jax.sharding import PartitionSpec as P


Z, ZLO, Y, X = 8, 4, 8, 4
ROW_GROUPS = [[z * Y + y for y in range(Y)] for z in range(ZLO)]
X_GROUPS = [[2 * x + c for x in range(X)] for c in range(2)]
OTHER_CORE = [(i, i ^ 1) for i in range(2 * X)]
PLANE = ("rep", "fs")


def z_shift(by):
    return [(z * Y + y, (z + by(z)) % Z * Y + y) for z in range(Z) for y in range(Y)]


FROM_NEXT = z_shift(lambda z: -1)
FROM_LAST = z_shift(lambda z: 1)
FROM_TWO = z_shift(lambda z: 2 if z % 2 == 0 else -2)


def spread(shard, axis, groups):
    copies = jnp.broadcast_to(shard[None], (len(groups[0]), *shard.shape))
    return lax.all_to_all(copies, axis, 0, 0, axis_index_groups=groups, tiled=True)


def gather_weight(piece):
    own = spread(piece, "fs", ROW_GROUPS).reshape(-1, piece.shape[1])
    return [
        own,
        lax.ppermute(own, PLANE, FROM_NEXT),
        lax.ppermute(own, PLANE, FROM_TWO),
        lax.ppermute(own, PLANE, FROM_LAST),
    ]


def rolled(a, by, width):
    n = a.shape[1] // width
    parts = [jnp.concatenate([a[:, width * k :], a[:, : width * k]], 1) for k in range(n)]
    out = parts[0]
    for k in range(1, n):
        out = jnp.where(by == k, parts[k], out)
    return out


def per_device(tokens, norm_gain, up_weight, up_scale, down_weight, down_scale):
    z = lax.axis_index("fs") // Y
    width = tokens.shape[1] // ZLO
    up = gather_weight(up_weight.astype(jnp.bfloat16))
    down = gather_weight((down_weight * down_scale).T.astype(jnp.bfloat16))
    values = tokens.astype(jnp.float32)
    normed = (
        values * lax.rsqrt(jnp.mean(values * values, axis=-1, keepdims=True) + 1e-06) * norm_gain
    ).astype(jnp.bfloat16)
    normed = rolled(normed, z, width)
    own = spread(normed, "tp", X_GROUPS).reshape(-1, normed.shape[1])
    other = lax.ppermute(own, "tp", OTHER_CORE)
    up_all = jnp.concatenate(up, 0)
    down_all = jnp.concatenate(down, 0)

    def mlp(rows):
        pre = jnp.dot(rows, up_all, preferred_element_type=jnp.float32) * up_scale
        hidden = jnp.square(jnp.maximum(pre, 0.0)).astype(jnp.bfloat16)
        return lax.dot_general(
            hidden, down_all, (((1,), (1,)), ((), ())), preferred_element_type=jnp.float32
        )

    for_other = lax.ppermute(mlp(other).astype(jnp.bfloat16), "tp", OTHER_CORE)
    pair = (mlp(own) + for_other.astype(jnp.float32)).astype(jnp.bfloat16)
    arrived = lax.all_to_all(
        pair.reshape(X, -1, pair.shape[1]), "tp", 0, 0, axis_index_groups=X_GROUPS, tiled=True
    )
    summed = arrived.astype(jnp.float32).sum(axis=0).astype(jnp.bfloat16)
    return rolled(summed, (ZLO - z) % ZLO, width)


def solution(mesh):
    return jax.shard_map(
        per_device,
        mesh=mesh,
        in_specs=(
            P(("rep", "fs", "tp"), None),
            P(),
            P("fs", "tp"),
            P(None, "tp"),
            P("tp", "fs"),
            P(None, "fs"),
        ),
        out_specs=P(("rep", "fs", "tp"), None),
        check_vma=False,
    )
```

```python
import jax
import jax.numpy as jnp
from jax import lax
from jax.sharding import PartitionSpec as P


Z, ZLO, Y, X = 8, 4, 8, 4
ROW_GROUPS = [[z * Y + y for y in range(Y)] for z in range(ZLO)]
X_GROUPS = [[2 * x + c for x in range(X)] for c in range(2)]
OTHER_CORE = [(i, i ^ 1) for i in range(2 * X)]
PLANE = ("rep", "fs")
F32, BF16 = jnp.float32, jnp.bfloat16


def z_shift(by):
    return [(z * Y + y, (z + by(z)) % Z * Y + y) for z in range(Z) for y in range(Y)]


def x_shift(by):
    return [(2 * x + c, (x + by(x)) % X * 2 + c) for x in range(X) for c in range(2)]


FROM_NEXT = z_shift(lambda z: -1)
FROM_LAST = z_shift(lambda z: 1)
FROM_TWO = z_shift(lambda z: 2 if z % 2 == 0 else -2)
X_NEXT = x_shift(lambda x: -1)
X_LAST = x_shift(lambda x: 1)
X_TWO = x_shift(lambda x: 2)


def swapped(blocks, axis, groups):
    return lax.all_to_all(blocks, axis, 0, 0, axis_index_groups=groups, tiled=True)


def spread(shard, axis, groups):
    return swapped(jnp.broadcast_to(shard[None], (len(groups[0]), *shard.shape)), axis, groups)


def rolled(a, by, width):
    n = a.shape[1] // width
    out = a
    for k in range(1, n):
        out = jnp.where(by == k, jnp.concatenate([a[:, width * k :], a[:, : width * k]], 1), out)
    return out


def body(tokens, norm_gain, up_weight, up_scale, down_weight, down_scale):
    z = lax.axis_index("fs") // Y
    x = lax.axis_index("tp") // 2
    rows, d = tokens.shape
    width = d // ZLO
    hidden_width = up_weight.shape[1]

    up_own = spread(up_weight.astype(BF16), "fs", ROW_GROUPS).reshape(width, hidden_width)
    down_piece = (down_weight * down_scale).T.astype(BF16)
    down_two = lax.ppermute(down_piece, PLANE, FROM_TWO)

    values = tokens.astype(F32)
    normed = (
        values * lax.rsqrt(jnp.mean(values * values, axis=-1, keepdims=True) + 1e-06) * norm_gain
    ).astype(BF16)
    normed = rolled(normed, z, width)
    near = [
        normed,
        lax.ppermute(normed, "tp", X_NEXT),
        lax.ppermute(normed, "tp", X_TWO),
        lax.ppermute(normed, "tp", X_LAST),
    ]
    own = jnp.zeros((X * rows, d), BF16)
    for k, block in enumerate(near):
        own = lax.dynamic_update_slice(own, block, (rows * ((x + k) % X), 0))
    other = lax.ppermute(own, "tp", OTHER_CORE)

    up_next = lax.ppermute(up_own, PLANE, FROM_NEXT)
    up_last = lax.ppermute(up_own, PLANE, FROM_LAST)
    half = width // 2
    up_two = jnp.concatenate(
        [lax.ppermute(up_next[:half], PLANE, FROM_NEXT), lax.ppermute(up_last[half:], PLANE, FROM_LAST)],
        0,
    )

    pieces, up_own = lax.optimization_barrier((jnp.stack([down_piece, down_two]), up_own))
    copies = jnp.broadcast_to(pieces[None], (Y, *pieces.shape))
    down_a = swapped(copies, "fs", ROW_GROUPS)
    first = lax.ppermute(down_a[: Y // 2], PLANE, FROM_NEXT)
    second = lax.ppermute(down_a[Y // 2 :], PLANE, FROM_LAST)
    down_b = jnp.stack(
        [jnp.concatenate([first[:, 0], second[:, 1]], 0), jnp.concatenate([first[:, 1], second[:, 0]], 0)]
    )
    down_b = down_b.reshape(2 * width, hidden_width)
    down_a = down_a.transpose(1, 0, 2, 3).reshape(2 * width, hidden_width)

    def hidden_of(t):
        pre = 0.0
        for k, block in enumerate([up_own, up_next, up_last, up_two]):
            place = (0, 1, 3, 2)[k]
            pre += jnp.dot(t[:, place * width : (place + 1) * width], block, preferred_element_type=F32)
        return jnp.square(jnp.maximum(pre * up_scale, 0.0)).astype(BF16)

    hidden_own, hidden_other = hidden_of(own), hidden_of(other)

    def chunk(down):
        def terms(hidden):
            return lax.dot_general(hidden, down, (((1,), (1,)), ((), ())), preferred_element_type=F32)

        arrived = lax.ppermute(terms(hidden_other).astype(BF16), "tp", OTHER_CORE)
        pair = (terms(hidden_own) + arrived.astype(F32)).astype(BF16)
        arrived = swapped(pair.reshape(X, rows, -1), "tp", X_GROUPS)
        return arrived.astype(F32).sum(axis=0).astype(BF16)

    out_a = chunk(down_a)
    out_b = chunk(down_b)
    summed = jnp.concatenate(
        [out_a[:, :width], out_b[:, :width], out_a[:, width:], out_b[:, width:]], 1
    )
    return rolled(summed, (ZLO - z) % ZLO, width)


def solution(mesh):
    return jax.shard_map(
        body,
        mesh=mesh,
        in_specs=(
            P(("rep", "fs", "tp"), None),
            P(),
            P("fs", "tp"),
            P(None, "tp"),
            P("tp", "fs"),
            P(None, "fs"),
        ),
        out_specs=P(("rep", "fs", "tp"), None),
        check_vma=False,
    )
```

```python
import jax
import jax.numpy as jnp
from jax import lax
from jax.sharding import PartitionSpec as P


Z, ZLO, Y, X = 8, 4, 8, 4
ROW_GROUPS = [[z * Y + y for y in range(Y)] for z in range(ZLO)]
X_GROUPS = [[2 * x + c for x in range(X)] for c in range(2)]
OTHER_CORE = [(i, i ^ 1) for i in range(2 * X)]
PLANE = ("rep", "fs")
F32, BF16 = jnp.float32, jnp.bfloat16


def z_shift(by):
    return [(z * Y + y, (z + by(z)) % Z * Y + y) for z in range(Z) for y in range(Y)]


def x_shift(by):
    return [(2 * x + c, (x + by(x)) % X * 2 + c) for x in range(X) for c in range(2)]


FROM_NEXT = z_shift(lambda z: -1)
FROM_LAST = z_shift(lambda z: 1)
FROM_TWO = z_shift(lambda z: 2 if z % 2 == 0 else -2)
X_NEXT = x_shift(lambda x: -1)
X_LAST = x_shift(lambda x: 1)
X_TWO = x_shift(lambda x: 2)


def swapped(blocks, axis, groups):
    return lax.all_to_all(blocks, axis, 0, 0, axis_index_groups=groups, tiled=True)


def spread(shard, axis, groups):
    copies = jnp.broadcast_to(shard[None], (len(groups[0]), *shard.shape))
    return swapped(copies, axis, groups).reshape(-1, shard.shape[1])


def rolled(a, by, width):
    n = a.shape[1] // width
    out = a
    for k in range(1, n):
        out = jnp.where(by == k, jnp.concatenate([a[:, width * k :], a[:, : width * k]], 1), out)
    return out


def body(tokens, norm_gain, up_weight, up_scale, down_weight, down_scale):
    z = lax.axis_index("fs") // Y
    x = lax.axis_index("tp") // 2
    rows, d = tokens.shape
    width = d // ZLO

    up_own = spread(up_weight.astype(BF16), "fs", ROW_GROUPS)
    down_piece = (down_weight * down_scale).T.astype(BF16)
    down_two = lax.ppermute(down_piece, PLANE, FROM_TWO)

    values = tokens.astype(F32)
    normed = (
        values * lax.rsqrt(jnp.mean(values * values, axis=-1, keepdims=True) + 1e-06) * norm_gain
    ).astype(BF16)
    normed = rolled(normed, z, width)
    near = [
        normed,
        lax.ppermute(normed, "tp", X_NEXT),
        lax.ppermute(normed, "tp", X_TWO),
        lax.ppermute(normed, "tp", X_LAST),
    ]
    own = jnp.zeros((X * rows, d), BF16)
    for k, block in enumerate(near):
        own = lax.dynamic_update_slice(own, block, (rows * ((x + k) % X), 0))
    other = lax.ppermute(own, "tp", OTHER_CORE)

    up = [
        up_own,
        lax.ppermute(up_own, PLANE, FROM_NEXT),
        lax.ppermute(up_own, PLANE, FROM_TWO),
        lax.ppermute(up_own, PLANE, FROM_LAST),
    ]
    up = lax.optimization_barrier(jnp.concatenate(up, 0))

    down_own = spread(down_piece, "fs", ROW_GROUPS)
    down_two, down_own = lax.optimization_barrier((down_two, down_own))
    down_two = spread(down_two, "fs", ROW_GROUPS)
    down_a = jnp.concatenate([down_own, down_two], 0)
    down_b = jnp.concatenate(
        [lax.ppermute(down_own, PLANE, FROM_NEXT), lax.ppermute(down_own, PLANE, FROM_LAST)], 0
    )
    down_a, down_b = lax.optimization_barrier(down_a), lax.optimization_barrier(down_b)

    def hidden_of(t):
        pre = jnp.dot(t, up, preferred_element_type=F32)
        return jnp.square(jnp.maximum(pre * up_scale, 0.0)).astype(BF16)

    hidden_own, hidden_other = hidden_of(own), hidden_of(other)

    def chunk(down):
        def terms(hidden):
            return lax.dot_general(hidden, down, (((1,), (1,)), ((), ())), preferred_element_type=F32)

        arrived = lax.ppermute(terms(hidden_other).astype(BF16), "tp", OTHER_CORE)
        pair = (terms(hidden_own) + arrived.astype(F32)).astype(BF16)
        arrived = swapped(pair.reshape(X, rows, -1), "tp", X_GROUPS)
        return arrived.astype(F32).sum(axis=0).astype(BF16)

    out_a = chunk(down_a)
    out_b = chunk(down_b)
    summed = jnp.concatenate(
        [out_a[:, :width], out_b[:, :width], out_a[:, width:], out_b[:, width:]], 1
    )
    return rolled(summed, (ZLO - z) % ZLO, width)


def solution(mesh):
    return jax.shard_map(
        body,
        mesh=mesh,
        in_specs=(
            P(("rep", "fs", "tp"), None),
            P(),
            P("fs", "tp"),
            P(None, "tp"),
            P("tp", "fs"),
            P(None, "fs"),
        ),
        out_specs=P(("rep", "fs", "tp"), None),
        check_vma=False,
    )
```

```python
import functools

import jax
import jax.numpy as jnp
from jax import lax
from jax.experimental import pallas as pl
from jax.experimental.pallas import tpu as pltpu
from jax.sharding import PartitionSpec as P


Z, ZLO, Y, X = 8, 4, 8, 4
ROW_GROUPS = [[z * Y + y for y in range(Y)] for z in range(ZLO)]
X_GROUPS = [[2 * x + c for x in range(X)] for c in range(2)]
OTHER_CORE = [(i, i ^ 1) for i in range(2 * X)]
PLANE = ("rep", "fs")
F32, BF16 = jnp.float32, jnp.bfloat16


def z_shift(by):
    return [(z * Y + y, (z + by(z)) % Z * Y + y) for z in range(Z) for y in range(Y)]


def x_shift(by):
    return [(2 * x + c, (x + by(x)) % X * 2 + c) for x in range(X) for c in range(2)]


FROM_NEXT = z_shift(lambda z: -1)
FROM_LAST = z_shift(lambda z: 1)
FROM_TWO = z_shift(lambda z: 2 if z % 2 == 0 else -2)
X_NEXT = x_shift(lambda x: -1)
X_LAST = x_shift(lambda x: 1)
X_TWO = x_shift(lambda x: 2)


def swapped(blocks, axis, groups):
    return lax.all_to_all(blocks, axis, 0, 0, axis_index_groups=groups, tiled=True)


def spread(shard, axis, groups):
    copies = jnp.broadcast_to(shard[None], (len(groups[0]), *shard.shape))
    return swapped(copies, axis, groups).reshape(-1, shard.shape[1])


def rolled(a, by, width):
    n = a.shape[1] // width
    out = a
    for k in range(1, n):
        out = jnp.where(by == k, jnp.concatenate([a[:, width * k :], a[:, : width * k]], 1), out)
    return out


def by_place_kernel(x_ref, *refs):
    *blocks, out = refs
    rows = blocks[0].shape[0]
    for k, block in enumerate(blocks):
        out[pl.ds(pl.multiple_of((x_ref[0] + k) % X * rows, rows), rows), :] = block[...]


def by_place(x, blocks):
    rows, columns = blocks[0].shape
    return pl.pallas_call(
        by_place_kernel,
        out_shape=jax.ShapeDtypeStruct((X * rows, columns), blocks[0].dtype),
        in_specs=[pl.BlockSpec(memory_space=pltpu.SMEM)] + [pl.BlockSpec(memory_space=pltpu.VMEM)] * X,
        out_specs=pl.BlockSpec(memory_space=pltpu.VMEM),
        cost_estimate=pl.CostEstimate(flops=1 << 28, bytes_accessed=4 * X * rows * columns, transcendentals=0),
        name="by_place",
    )(x[None], *blocks)


def from_place_kernel(x_ref, a, *outs):
    rows = outs[0].shape[0]
    for k, out in enumerate(outs):
        out[...] = a[pl.ds(pl.multiple_of((x_ref[0] + k) % X * rows, rows), rows), :]


def from_place(x, a):
    shape = (a.shape[0] // X, a.shape[1])
    return pl.pallas_call(
        from_place_kernel,
        out_shape=[jax.ShapeDtypeStruct(shape, a.dtype)] * X,
        in_specs=[pl.BlockSpec(memory_space=pltpu.SMEM), pl.BlockSpec(memory_space=pltpu.VMEM)],
        out_specs=[pl.BlockSpec(memory_space=pltpu.VMEM)] * X,
        cost_estimate=pl.CostEstimate(flops=1 << 28, bytes_accessed=4 * a.size, transcendentals=0),
        name="from_place",
    )(x[None], a)


TILE = 256


def hidden_kernel(half, own, other, u0, u1, u2, u3, scale, out):
    def write(rows):
        width = u0.shape[0]
        pre = jnp.dot(rows[:, :width], u0[...], preferred_element_type=F32)
        for k, block in enumerate((u1, u2, u3), 1):
            pre += jnp.dot(rows[:, k * width : (k + 1) * width], block[...], preferred_element_type=F32)
        out[...] = jnp.square(jnp.maximum(pre * scale[...], 0.0)).astype(out.dtype)

    @pl.when(pl.program_id(0) < half)
    def _():
        write(own)

    @pl.when(pl.program_id(0) >= half)
    def _():
        write(other)


def hidden_of(own, other, up, scale):
    rows, d = own.shape
    width, columns = up[0].shape
    half = rows // TILE
    whole = pl.BlockSpec((width, columns), lambda i: (0, 0))
    return pl.pallas_call(
        functools.partial(hidden_kernel, half),
        grid=(2 * half,),
        out_shape=jax.ShapeDtypeStruct((2 * rows, columns), BF16),
        in_specs=[
            pl.BlockSpec((TILE, d), lambda i: (jnp.minimum(i, half - 1), 0)),
            pl.BlockSpec((TILE, d), lambda i: (jnp.maximum(i - half, 0), 0)),
            *([whole] * ZLO),
            pl.BlockSpec((1, columns), lambda i: (0, 0)),
        ],
        out_specs=pl.BlockSpec((TILE, columns), lambda i: (i, 0)),
        cost_estimate=pl.CostEstimate(
            flops=4 * rows * d * columns, bytes_accessed=4 * rows * d + 2 * d * columns + 4 * rows * columns, transcendentals=0
        ),
        name="hidden",
    )(own, other, *up, scale)


def body(tokens, norm_gain, up_weight, up_scale, down_weight, down_scale):
    z = lax.axis_index("fs") // Y
    x = lax.axis_index("tp") // 2
    rows, d = tokens.shape
    width = d // ZLO

    up_own = spread(up_weight.astype(BF16), "fs", ROW_GROUPS)
    down_piece = (down_weight * down_scale).T.astype(BF16)
    values = tokens.astype(F32)
    normed = (
        values * lax.rsqrt(jnp.mean(values * values, axis=-1, keepdims=True) + 1e-06) * norm_gain
    ).astype(BF16)
    normed = rolled(normed, z, width)
    near = [
        normed,
        lax.ppermute(normed, "tp", X_NEXT),
        lax.ppermute(normed, "tp", X_TWO),
        lax.ppermute(normed, "tp", X_LAST),
    ]
    own = by_place(x, near)
    other = lax.ppermute(own, "tp", OTHER_CORE)

    up = [
        up_own,
        lax.ppermute(up_own, PLANE, FROM_NEXT),
        lax.ppermute(up_own, PLANE, FROM_TWO),
        lax.ppermute(up_own, PLANE, FROM_LAST),
    ]
    down_piece, _ = lax.optimization_barrier((down_piece, up_own))
    down_own = spread(down_piece, "fs", ROW_GROUPS)
    down_b = jnp.concatenate([lax.ppermute(down_own, PLANE, FROM_NEXT), lax.ppermute(down_own, PLANE, FROM_LAST)], 0)
    down_b = lax.optimization_barrier(down_b)
    down_c = lax.ppermute(down_own, PLANE, FROM_TWO)

    hidden = hidden_of(own, other, up, up_scale)
    hidden_own, hidden_other = hidden[: X * rows], hidden[X * rows :]

    def pair_of(down):
        def terms(hidden):
            return lax.dot_general(hidden, down, (((1,), (1,)), ((), ())), preferred_element_type=F32)

        arrived = lax.ppermute(terms(hidden_other).astype(BF16), "tp", OTHER_CORE)
        return (terms(hidden_own) + arrived.astype(F32)).astype(BF16)

    def exchanged(pair):
        arrived = swapped(pair.reshape(X, rows, -1), "tp", X_GROUPS)
        return arrived.astype(F32).sum(axis=0).astype(BF16)

    out_a = exchanged(pair_of(down_own))
    out_b = exchanged(pair_of(down_b))
    mine, for_next, for_two, for_last = from_place(x, pair_of(down_c))
    out_c = mine.astype(F32)
    out_c += lax.ppermute(for_next, "tp", X_LAST).astype(F32)
    out_c += lax.ppermute(for_two, "tp", X_TWO).astype(F32)
    out_c += lax.ppermute(for_last, "tp", X_NEXT).astype(F32)
    summed = jnp.concatenate([out_a, out_b[:, :width], out_c.astype(BF16), out_b[:, width:]], 1)
    return rolled(summed, (ZLO - z) % ZLO, width)


def solution(mesh):
    return jax.shard_map(
        body,
        mesh=mesh,
        in_specs=(
            P(("rep", "fs", "tp"), None),
            P(),
            P("fs", "tp"),
            P(None, "tp"),
            P("tp", "fs"),
            P(None, "fs"),
        ),
        out_specs=P(("rep", "fs", "tp"), None),
        check_vma=False,
    )
```

```python
import functools

import jax
import jax.numpy as jnp
from jax import lax
from jax.experimental import pallas as pl
from jax.experimental.pallas import tpu as pltpu
from jax.sharding import PartitionSpec as P


Z, ZLO, Y, X = 8, 4, 8, 4
ROW_GROUPS = [[z * Y + y for y in range(Y)] for z in range(ZLO)]
X_GROUPS = [[2 * x + c for x in range(X)] for c in range(2)]
OTHER_CORE = [(i, i ^ 1) for i in range(2 * X)]
PLANE = ("rep", "fs")
F32, BF16 = jnp.float32, jnp.bfloat16


def z_shift(by):
    return [(z * Y + y, (z + by(z)) % Z * Y + y) for z in range(Z) for y in range(Y)]


def x_shift(by):
    return [(2 * x + c, (x + by(x)) % X * 2 + c) for x in range(X) for c in range(2)]


FROM_NEXT = z_shift(lambda z: -1)
FROM_LAST = z_shift(lambda z: 1)
FROM_TWO = z_shift(lambda z: 2 if z % 2 == 0 else -2)
X_NEXT = x_shift(lambda x: -1)
X_LAST = x_shift(lambda x: 1)
X_TWO = x_shift(lambda x: 2)


def swapped(blocks, axis, groups):
    return lax.all_to_all(blocks, axis, 0, 0, axis_index_groups=groups, tiled=True)


def spread(shard, axis, groups):
    copies = jnp.broadcast_to(shard[None], (len(groups[0]), *shard.shape))
    return swapped(copies, axis, groups).reshape(-1, shard.shape[1])


def rolled(a, by, width):
    n = a.shape[1] // width
    out = a
    for k in range(1, n):
        out = jnp.where(by == k, jnp.concatenate([a[:, width * k :], a[:, : width * k]], 1), out)
    return out


def by_place_kernel(x_ref, *refs):
    *blocks, out = refs
    rows = blocks[0].shape[0]
    for k, block in enumerate(blocks):
        out[pl.ds(pl.multiple_of((x_ref[0] + k) % X * rows, rows), rows), :] = block[...]


def by_place(x, blocks):
    rows, columns = blocks[0].shape
    return pl.pallas_call(
        by_place_kernel,
        out_shape=jax.ShapeDtypeStruct((X * rows, columns), blocks[0].dtype),
        in_specs=[pl.BlockSpec(memory_space=pltpu.SMEM)] + [pl.BlockSpec(memory_space=pltpu.VMEM)] * X,
        out_specs=pl.BlockSpec(memory_space=pltpu.VMEM),
        cost_estimate=pl.CostEstimate(flops=1 << 28, bytes_accessed=4 * X * rows * columns, transcendentals=0),
        compiler_params=pltpu.CompilerParams(vmem_limit_bytes=8 << 20),
        name="by_place",
    )(x[None], *blocks)


TILE = 256


def hidden_kernel(half, own, other, u0, u1, u2, u3, scale, out, up, sems):
    step = pl.program_id(0)

    @pl.when(step == 0)
    def _():
        width = u0.shape[0]
        copies = [
            pltpu.make_async_copy(block, up.at[pl.ds(k * width, width)], sems.at[k])
            for k, block in enumerate((u0, u1, u2, u3))
        ]
        for copy in copies:
            copy.start()
        for copy in copies:
            copy.wait()

    def write(rows):
        pre = jnp.dot(rows[...], up[...], preferred_element_type=F32)
        out[...] = jnp.square(jnp.maximum(pre * scale[...], 0.0)).astype(out.dtype)

    @pl.when(step < half)
    def _():
        write(other)

    @pl.when(step >= half)
    def _():
        write(own)


def hidden_of(own, other, up, scale):
    rows, d = own.shape
    _, columns = up[0].shape
    half = rows // TILE
    return pl.pallas_call(
        functools.partial(hidden_kernel, half),
        grid=(2 * half,),
        out_shape=jax.ShapeDtypeStruct((2 * rows, columns), BF16),
        in_specs=[
            pl.BlockSpec((TILE, d), lambda i: (jnp.maximum(i - half, 0), 0)),
            pl.BlockSpec((TILE, d), lambda i: (jnp.minimum(i, half - 1), 0)),
            *([pl.BlockSpec(memory_space=pl.ANY)] * ZLO),
            pl.BlockSpec((1, columns), lambda i: (0, 0)),
        ],
        out_specs=pl.BlockSpec((TILE, columns), lambda i: (i, 0)),
        scratch_shapes=[pltpu.VMEM((d, columns), BF16), pltpu.SemaphoreType.DMA((ZLO,))],
        compiler_params=pltpu.CompilerParams(vmem_limit_bytes=16 << 20),
        cost_estimate=pl.CostEstimate(
            flops=4 * rows * d * columns, bytes_accessed=4 * rows * d + 2 * d * columns + 4 * rows * columns, transcendentals=0
        ),
        name="hidden",
    )(own, other, *up, scale)


def body(tokens, norm_gain, up_weight, up_scale, down_weight, down_scale):
    z = lax.axis_index("fs") // Y
    x = lax.axis_index("tp") // 2
    rows, d = tokens.shape
    width = d // ZLO

    up_own = spread(up_weight.astype(BF16), "fs", ROW_GROUPS)
    down_piece = (down_weight * down_scale).T.astype(BF16)
    down_two = lax.ppermute(down_piece, PLANE, FROM_TWO)

    values = tokens.astype(F32)
    normed = (
        values * lax.rsqrt(jnp.mean(values * values, axis=-1, keepdims=True) + 1e-06) * norm_gain
    ).astype(BF16)
    normed = rolled(normed, z, width)
    near = [
        normed,
        lax.ppermute(normed, "tp", X_NEXT),
        lax.ppermute(normed, "tp", X_TWO),
        lax.ppermute(normed, "tp", X_LAST),
    ]
    own = by_place(x, near)
    other = lax.ppermute(own, "tp", OTHER_CORE)

    up = [
        up_own,
        lax.ppermute(up_own, PLANE, FROM_NEXT),
        lax.ppermute(up_own, PLANE, FROM_TWO),
        lax.ppermute(up_own, PLANE, FROM_LAST),
    ]
    down_own = spread(down_piece, "fs", ROW_GROUPS)
    down_two, down_own = lax.optimization_barrier((down_two, down_own))
    down_two = spread(down_two, "fs", ROW_GROUPS)
    down_a = jnp.concatenate([down_own, down_two], 0)
    down_b = jnp.concatenate([lax.ppermute(down_own, PLANE, FROM_NEXT), lax.ppermute(down_own, PLANE, FROM_LAST)], 0)
    down_a, down_b = lax.optimization_barrier(down_a), lax.optimization_barrier(down_b)

    hidden = hidden_of(own, other, up, up_scale)
    hidden_other, hidden_own = hidden[: X * rows], hidden[X * rows :]

    def chunk(down):
        def terms(hidden):
            return lax.dot_general(hidden, down, (((1,), (1,)), ((), ())), preferred_element_type=F32)

        arrived = lax.ppermute(terms(hidden_other).astype(BF16), "tp", OTHER_CORE)
        pair = (terms(hidden_own) + arrived.astype(F32)).astype(BF16)
        arrived = swapped(pair.reshape(X, rows, -1), "tp", X_GROUPS)
        return arrived.astype(F32).sum(axis=0).astype(BF16)

    out_a = chunk(down_a)
    out_b = chunk(down_b)
    summed = jnp.concatenate(
        [out_a[:, :width], out_b[:, :width], out_a[:, width:], out_b[:, width:]], 1
    )
    return rolled(summed, (ZLO - z) % ZLO, width)


def solution(mesh):
    return jax.shard_map(
        body,
        mesh=mesh,
        in_specs=(
            P(("rep", "fs", "tp"), None),
            P(),
            P("fs", "tp"),
            P(None, "tp"),
            P("tp", "fs"),
            P(None, "fs"),
        ),
        out_specs=P(("rep", "fs", "tp"), None),
        check_vma=False,
    )
```

```python
import functools

import jax
import jax.numpy as jnp
from jax import lax
from jax.experimental import pallas as pl
from jax.experimental.pallas import tpu as pltpu
from jax.sharding import PartitionSpec as P


Z, ZLO, Y, X = 8, 4, 8, 4
ROW_GROUPS = [[z * Y + y for y in range(Y)] for z in range(ZLO)]
X_GROUPS = [[2 * x + c for x in range(X)] for c in range(2)]
OTHER_CORE = [(i, i ^ 1) for i in range(2 * X)]
PLANE = ("rep", "fs")
F32, BF16 = jnp.float32, jnp.bfloat16


def z_shift(by):
    return [(z * Y + y, (z + by(z)) % Z * Y + y) for z in range(Z) for y in range(Y)]


def x_shift(by):
    return [(2 * x + c, (x + by(x)) % X * 2 + c) for x in range(X) for c in range(2)]


FROM_NEXT = z_shift(lambda z: -1)
FROM_LAST = z_shift(lambda z: 1)
FROM_TWO = z_shift(lambda z: 2 if z % 2 == 0 else -2)
X_NEXT = x_shift(lambda x: -1)
X_LAST = x_shift(lambda x: 1)
X_TWO = x_shift(lambda x: 2)


def swapped(blocks, axis, groups):
    return lax.all_to_all(blocks, axis, 0, 0, axis_index_groups=groups, tiled=True)


def rolled(a, by, width):
    n = a.shape[1] // width
    out = a
    for k in range(1, n):
        out = jnp.where(by == k, jnp.concatenate([a[:, width * k :], a[:, : width * k]], 1), out)
    return out


VMEM = pl.BlockSpec(memory_space=pltpu.VMEM)
SMEM = pl.BlockSpec(memory_space=pltpu.SMEM)


def cost(flops, *arrays):
    return pl.CostEstimate(flops=flops, bytes_accessed=sum(a.size * a.dtype.itemsize for a in arrays), transcendentals=0)


def copies_kernel(*refs):
    *shards, out = refs
    for k, shard in enumerate(shards):
        block = shard[...].astype(out.dtype)
        for i in range(out.shape[0]):
            out[i, k] = block


def copies_of(shards):
    out = jax.ShapeDtypeStruct((Y, len(shards), *shards[0].shape), BF16)
    return pl.pallas_call(
        copies_kernel,
        out_shape=out,
        in_specs=[VMEM] * len(shards),
        out_specs=VMEM,
        compiler_params=pltpu.CompilerParams(vmem_limit_bytes=8 << 20),
        cost_estimate=cost(1 << 28, out, *shards),
        name="copies",
    )(*shards)


def split_kernel(blocks, own, both):
    rows = blocks.shape[2]
    width = own.shape[0]
    for y in range(blocks.shape[0]):
        own[y * rows : (y + 1) * rows] = both[y * rows : (y + 1) * rows] = blocks[y, 0]
        both[width + y * rows : width + (y + 1) * rows] = blocks[y, 1]


def split(blocks):
    count, _, rows, columns = blocks.shape
    own = jax.ShapeDtypeStruct((count * rows, columns), BF16)
    both = jax.ShapeDtypeStruct((2 * count * rows, columns), BF16)
    return pl.pallas_call(
        split_kernel,
        out_shape=[own, both],
        in_specs=[VMEM],
        out_specs=[VMEM] * 2,
        compiler_params=pltpu.CompilerParams(vmem_limit_bytes=8 << 20),
        cost_estimate=cost(1 << 28, own, both, blocks),
        name="split",
    )(blocks)


def by_place_kernel(x_ref, *refs):
    *blocks, out = refs
    rows = blocks[0].shape[0]
    for k, block in enumerate(blocks):
        out[pl.ds(pl.multiple_of((x_ref[0] + k) % X * rows, rows), rows), :] = block[...]


def by_place(x, blocks):
    rows, columns = blocks[0].shape
    return pl.pallas_call(
        by_place_kernel,
        out_shape=jax.ShapeDtypeStruct((X * rows, columns), blocks[0].dtype),
        in_specs=[SMEM] + [VMEM] * X,
        out_specs=VMEM,
        cost_estimate=cost(1 << 28, *blocks, *blocks),
        compiler_params=pltpu.CompilerParams(vmem_limit_bytes=8 << 20),
        name="by_place",
    )(x[None], *blocks)


TILE = 256


def hidden_kernel(half, other, own, u0, u1, u2, u3, scale, down_ref, hidden, terms, up, down, sems):
    step = pl.program_id(0)

    @pl.when(step == 0)
    def _():
        width = u0.shape[0]
        fetches = [
            pltpu.make_async_copy(block, up.at[pl.ds(k * width, width)], sems.at[k])
            for k, block in enumerate((u0, u1, u2, u3))
        ]
        fetches.append(pltpu.make_async_copy(down_ref, down, sems.at[len(fetches)]))
        for fetch in fetches:
            fetch.start()
        for fetch in fetches:
            fetch.wait()

    def hidden_of(rows):
        pre = jnp.dot(rows[...], up[...], preferred_element_type=F32)
        return jnp.square(jnp.maximum(pre * scale[...], 0.0)).astype(BF16)

    @pl.when(step < half)
    def _():
        tile = hidden_of(other)
        hidden[...] = tile
        terms[...] = lax.dot_general(
            tile, down[...], (((1,), (1,)), ((), ())), preferred_element_type=F32
        ).astype(BF16)

    @pl.when(step >= half)
    def _():
        hidden[...] = hidden_of(own)


def hidden_of(other, own, up, scale, down):
    rows, d = own.shape
    _, columns = up[0].shape
    half = rows // TILE
    hidden = jax.ShapeDtypeStruct((2 * rows, columns), BF16)
    terms = jax.ShapeDtypeStruct((rows, down.shape[0]), BF16)
    anywhere = pl.BlockSpec(memory_space=pl.ANY)
    return pl.pallas_call(
        functools.partial(hidden_kernel, half),
        grid=(2 * half,),
        out_shape=[hidden, terms],
        in_specs=[
            pl.BlockSpec((TILE, d), lambda i: (jnp.minimum(i, half - 1), 0)),
            pl.BlockSpec((TILE, d), lambda i: (jnp.maximum(i - half, 0), 0)),
            *([anywhere] * ZLO),
            pl.BlockSpec((1, columns), lambda i: (0, 0)),
            anywhere,
        ],
        out_specs=[
            pl.BlockSpec((TILE, columns), lambda i: (i, 0)),
            pl.BlockSpec((TILE, down.shape[0]), lambda i: (jnp.minimum(i, half - 1), 0)),
        ],
        scratch_shapes=[
            pltpu.VMEM((d, columns), BF16),
            pltpu.VMEM(down.shape, BF16),
            pltpu.SemaphoreType.DMA((ZLO + 1,)),
        ],
        compiler_params=pltpu.CompilerParams(vmem_limit_bytes=24 << 20),
        cost_estimate=cost(4 * rows * d * columns, own, other, *up, down, hidden, terms),
        name="hidden",
    )(other, own, *up, scale, down)


def body(tokens, norm_gain, up_weight, up_scale, down_weight, down_scale):
    z = lax.axis_index("fs") // Y
    x = lax.axis_index("tp") // 2
    rows, d = tokens.shape
    width = d // ZLO
    hidden_width = up_weight.shape[1]

    copies = copies_of([up_weight])
    up_own = swapped(copies[:, 0], "fs", ROW_GROUPS).reshape(width, hidden_width)
    down_piece = (down_weight * down_scale).T.astype(BF16)
    down_two = lax.ppermute(down_piece, PLANE, FROM_TWO)

    values = tokens.astype(F32)
    normed = (
        values * lax.rsqrt(jnp.mean(values * values, axis=-1, keepdims=True) + 1e-06) * norm_gain
    ).astype(BF16)
    normed = rolled(normed, z, width)
    near = [
        normed,
        lax.ppermute(normed, "tp", X_NEXT),
        lax.ppermute(normed, "tp", X_TWO),
        lax.ppermute(normed, "tp", X_LAST),
    ]
    own = by_place(x, near)
    other = lax.ppermute(own, "tp", OTHER_CORE)

    up = [
        up_own,
        lax.ppermute(up_own, PLANE, FROM_NEXT),
        lax.ppermute(up_own, PLANE, FROM_TWO),
        lax.ppermute(up_own, PLANE, FROM_LAST),
    ]
    copies = copies_of([down_piece, down_two])
    down_own, down_a = split(swapped(copies, "fs", ROW_GROUPS))
    down_b = jnp.concatenate(
        [lax.ppermute(down_own, PLANE, FROM_NEXT), lax.ppermute(down_own, PLANE, FROM_LAST)], 0
    )
    down_b = lax.optimization_barrier(down_b)

    hidden, for_other = hidden_of(other, own, up, up_scale, down_a)
    hidden_other, hidden_own = hidden[: X * rows], hidden[X * rows :]

    def terms(hidden, down):
        return lax.dot_general(hidden, down, (((1,), (1,)), ((), ())), preferred_element_type=F32)

    def chunk(down, for_other):
        arrived = lax.ppermute(for_other, "tp", OTHER_CORE)
        pair = (terms(hidden_own, down) + arrived.astype(F32)).astype(BF16)
        arrived = swapped(pair.reshape(X, rows, -1), "tp", X_GROUPS)
        return arrived.astype(F32).sum(axis=0).astype(BF16)

    out_a = chunk(down_a, for_other)
    out_b = chunk(down_b, terms(hidden_other, down_b).astype(BF16))
    summed = jnp.concatenate(
        [out_a[:, :width], out_b[:, :width], out_a[:, width:], out_b[:, width:]], 1
    )
    return rolled(summed, (ZLO - z) % ZLO, width)


def solution(mesh):
    return jax.shard_map(
        body,
        mesh=mesh,
        in_specs=(
            P(("rep", "fs", "tp"), None),
            P(),
            P("fs", "tp"),
            P(None, "tp"),
            P("tp", "fs"),
            P(None, "fs"),
        ),
        out_specs=P(("rep", "fs", "tp"), None),
        check_vma=False,
    )
```

```python
import functools

import jax
import jax.numpy as jnp
from jax import lax
from jax.experimental import pallas as pl
from jax.experimental.pallas import tpu as pltpu
from jax.sharding import PartitionSpec as P


Z, ZLO, Y, X = 8, 4, 8, 4
ROW_GROUPS = [[z * Y + y for y in range(Y)] for z in range(ZLO)]
X_GROUPS = [[2 * x + c for x in range(X)] for c in range(2)]
OTHER_CORE = [(i, i ^ 1) for i in range(2 * X)]
PLANE = ("rep", "fs")
F32, BF16 = jnp.float32, jnp.bfloat16


def z_shift(by):
    return [(z * Y + y, (z + by(z)) % Z * Y + y) for z in range(Z) for y in range(Y)]


def x_shift(by):
    return [(2 * x + c, (x + by(x)) % X * 2 + c) for x in range(X) for c in range(2)]


FROM_NEXT = z_shift(lambda z: -1)
FROM_LAST = z_shift(lambda z: 1)
FROM_TWO = z_shift(lambda z: 2 if z % 2 == 0 else -2)
X_NEXT = x_shift(lambda x: -1)
X_LAST = x_shift(lambda x: 1)
X_TWO = x_shift(lambda x: 2)


def swapped(blocks, axis, groups):
    return lax.all_to_all(blocks, axis, 0, 0, axis_index_groups=groups, tiled=True)


def rolled(a, by, width):
    n = a.shape[1] // width
    out = a
    for k in range(1, n):
        out = jnp.where(by == k, jnp.concatenate([a[:, width * k :], a[:, : width * k]], 1), out)
    return out


VMEM = pl.BlockSpec(memory_space=pltpu.VMEM)
HBM = pl.BlockSpec(memory_space=pltpu.HBM)
SMEM = pl.BlockSpec(memory_space=pltpu.SMEM)


def cost(flops, *arrays):
    return pl.CostEstimate(flops=flops, bytes_accessed=sum(a.size * a.dtype.itemsize for a in arrays), transcendentals=0)


def copies_kernel(*refs):
    *shards, out = refs
    for k, shard in enumerate(shards):
        block = shard[...].astype(out.dtype)
        for i in range(out.shape[0]):
            out[i, k] = block


def copies_of(shards):
    out = jax.ShapeDtypeStruct((Y, len(shards), *shards[0].shape), BF16)
    return pl.pallas_call(
        copies_kernel,
        out_shape=out,
        in_specs=[VMEM] * len(shards),
        out_specs=VMEM,
        compiler_params=pltpu.CompilerParams(vmem_limit_bytes=8 << 20),
        cost_estimate=cost(1 << 28, out, *shards),
        name="copies",
    )(*shards)


def split_kernel(blocks, own, both):
    rows = blocks.shape[2]
    width = own.shape[0]
    for y in range(blocks.shape[0]):
        own[y * rows : (y + 1) * rows] = both[y * rows : (y + 1) * rows] = blocks[y, 0]
        both[width + y * rows : width + (y + 1) * rows] = blocks[y, 1]


def split(blocks):
    count, _, rows, columns = blocks.shape
    own = jax.ShapeDtypeStruct((count * rows, columns), BF16)
    both = jax.ShapeDtypeStruct((2 * count * rows, columns), BF16)
    return pl.pallas_call(
        split_kernel,
        out_shape=[own, both],
        in_specs=[VMEM],
        out_specs=[VMEM] * 2,
        compiler_params=pltpu.CompilerParams(vmem_limit_bytes=8 << 20),
        cost_estimate=cost(1 << 28, own, both, blocks),
        name="split",
    )(blocks)


def by_place_kernel(x_ref, *refs):
    *blocks, out, sems = refs
    rows = blocks[0].shape[0]
    fetches = [
        pltpu.make_async_copy(
            block, out.at[pl.ds(pl.multiple_of((x_ref[0] + k) % X * rows, rows), rows)], sems.at[k]
        )
        for k, block in enumerate(blocks)
    ]
    for fetch in fetches:
        fetch.start()
    for fetch in fetches:
        fetch.wait()


def by_place(x, blocks):
    rows, columns = blocks[0].shape
    return pl.pallas_call(
        by_place_kernel,
        out_shape=jax.ShapeDtypeStruct((X * rows, columns), blocks[0].dtype),
        in_specs=[SMEM] + [HBM] * X,
        out_specs=VMEM,
        scratch_shapes=[pltpu.SemaphoreType.DMA((X,))],
        cost_estimate=cost(1 << 28, *blocks, *blocks),
        compiler_params=pltpu.CompilerParams(vmem_limit_bytes=4 << 20),
        name="by_place",
    )(x[None], *blocks)


TILE = 256


def fetched(sources, target, sems):
    @pl.when(pl.program_id(0) == 0)
    def _():
        rows = sources[0].shape[0]
        fetches = [
            pltpu.make_async_copy(source, target.at[pl.ds(k * rows, rows)], sems.at[k])
            for k, source in enumerate(sources)
        ]
        for fetch in fetches:
            fetch.start()
        for fetch in fetches:
            fetch.wait()


def early_kernel(half, other, own, u0, u1, u3, early, up, sems):
    fetched((u0, u1, u3), up, sems)
    width, columns = u0.shape

    def write(rows):
        pre = jnp.dot(rows[:, : 2 * width], up[: 2 * width], preferred_element_type=F32)
        pre += jnp.dot(rows[:, 3 * width :], up[2 * width :], preferred_element_type=F32)
        early[:, :columns] = pre.astype(early.dtype)
        early[:, columns:] = rows[:, 2 * width : 3 * width]

    @pl.when(pl.program_id(0) < half)
    def _():
        write(other)

    @pl.when(pl.program_id(0) >= half)
    def _():
        write(own)


def early_of(other, own, blocks):
    rows, d = own.shape
    width, columns = blocks[0].shape
    half = rows // TILE
    shape = (2 * rows, columns + width)
    return pl.pallas_call(
        functools.partial(early_kernel, half),
        grid=(2 * half,),
        out_shape=pltpu.HBM(shape, BF16),
        in_specs=[
            pl.BlockSpec((TILE, d), lambda i: (jnp.minimum(i, half - 1), 0)),
            pl.BlockSpec((TILE, d), lambda i: (jnp.maximum(i - half, 0), 0)),
            *([HBM] * len(blocks)),
        ],
        out_specs=pl.BlockSpec((TILE, shape[1]), lambda i: (i, 0)),
        scratch_shapes=[
            pltpu.VMEM((len(blocks) * width, columns), BF16),
            pltpu.SemaphoreType.DMA((len(blocks),)),
        ],
        compiler_params=pltpu.CompilerParams(vmem_limit_bytes=16 << 20),
        cost_estimate=cost(4 * rows * 3 * width * columns, own, other, *blocks),
        name="early",
    )(other, own, *blocks)


def late_kernel(early, u2, scale, hidden, tiles, up, sems):
    step, steps = pl.program_id(0), early.shape[0] // TILE
    columns = hidden.shape[1]

    def fetch(i):
        rows = pl.ds(i * TILE if isinstance(i, int) else pl.multiple_of(i * TILE, TILE), TILE)
        return pltpu.make_async_copy(early.at[rows], tiles.at[rows], sems.at[i])

    @pl.when(step == 0)
    def _():
        block = pltpu.make_async_copy(u2, up, sems.at[steps])
        block.start()
        for i in range(steps):
            fetch(i).start()
        block.wait()

    fetch(step).wait()
    tile = tiles.at[pl.ds(pl.multiple_of(step * TILE, TILE), TILE)]
    pre = jnp.dot(tile[:, columns:], up[...], preferred_element_type=F32) + tile[:, :columns].astype(F32)
    hidden[...] = jnp.square(jnp.maximum(pre * scale[...], 0.0)).astype(BF16)


def late_of(early, block, scale):
    width, columns = block.shape
    steps = early.shape[0] // TILE
    out = jax.ShapeDtypeStruct((early.shape[0], columns), BF16)
    return pl.pallas_call(
        late_kernel,
        grid=(steps,),
        out_shape=out,
        in_specs=[HBM, HBM, pl.BlockSpec((1, columns), lambda i: (0, 0))],
        out_specs=pl.BlockSpec((TILE, columns), lambda i: (i, 0)),
        scratch_shapes=[
            pltpu.VMEM(early.shape, BF16),
            pltpu.VMEM((width, columns), BF16),
            pltpu.SemaphoreType.DMA((steps + 1,)),
        ],
        compiler_params=pltpu.CompilerParams(vmem_limit_bytes=12 << 20),
        cost_estimate=cost(2 * early.shape[0] * width * columns, early, block, out),
        name="late",
    )(early, block, scale)


def body(tokens, norm_gain, up_weight, up_scale, down_weight, down_scale):
    z = lax.axis_index("fs") // Y
    x = lax.axis_index("tp") // 2
    rows, d = tokens.shape
    width = d // ZLO
    hidden_width = up_weight.shape[1]

    copies = copies_of([up_weight])
    up_own = swapped(copies[:, 0], "fs", ROW_GROUPS).reshape(width, hidden_width)
    down_piece = (down_weight * down_scale).T.astype(BF16)
    down_two = lax.ppermute(down_piece, PLANE, FROM_TWO)

    values = tokens.astype(F32)
    normed = (
        values * lax.rsqrt(jnp.mean(values * values, axis=-1, keepdims=True) + 1e-06) * norm_gain
    ).astype(BF16)
    normed = rolled(normed, z, width)
    near = [
        normed,
        lax.ppermute(normed, "tp", X_NEXT),
        lax.ppermute(normed, "tp", X_TWO),
        lax.ppermute(normed, "tp", X_LAST),
    ]
    own = by_place(x, near)
    other = lax.ppermute(own, "tp", OTHER_CORE)

    up_next = lax.ppermute(up_own, PLANE, FROM_NEXT)
    up_last = lax.ppermute(up_own, PLANE, FROM_LAST)
    up_two = lax.ppermute(up_own, PLANE, FROM_TWO)

    copies = copies_of([down_piece, down_two])
    down_own, down_a = split(swapped(copies, "fs", ROW_GROUPS))
    down_b = jnp.concatenate(
        [lax.ppermute(down_own, PLANE, FROM_NEXT), lax.ppermute(down_own, PLANE, FROM_LAST)], 0
    )
    down_b = lax.optimization_barrier(down_b)

    early = early_of(other, own, (up_own, up_next, up_last))
    hidden = late_of(early, up_two, up_scale)
    hidden_other, hidden_own = hidden[: X * rows], hidden[X * rows :]

    def terms(hidden, down):
        return lax.dot_general(hidden, down, (((1,), (1,)), ((), ())), preferred_element_type=F32)

    def chunk(down, for_other):
        arrived = lax.ppermute(for_other, "tp", OTHER_CORE)
        pair = (terms(hidden_own, down) + arrived.astype(F32)).astype(BF16)
        arrived = swapped(pair.reshape(X, rows, -1), "tp", X_GROUPS)
        return arrived.astype(F32).sum(axis=0).astype(BF16)

    out_a = chunk(down_a, terms(hidden_other, down_a).astype(BF16))
    out_b = chunk(down_b, terms(hidden_other, down_b).astype(BF16))
    summed = jnp.concatenate(
        [out_a[:, :width], out_b[:, :width], out_a[:, width:], out_b[:, width:]], 1
    )
    return rolled(summed, (ZLO - z) % ZLO, width)


def solution(mesh):
    return jax.shard_map(
        body,
        mesh=mesh,
        in_specs=(
            P(("rep", "fs", "tp"), None),
            P(),
            P("fs", "tp"),
            P(None, "tp"),
            P("tp", "fs"),
            P(None, "fs"),
        ),
        out_specs=P(("rep", "fs", "tp"), None),
        check_vma=False,
    )
```

```python
import functools

import jax
import jax.numpy as jnp
from jax import lax
from jax.experimental import pallas as pl
from jax.experimental.pallas import tpu as pltpu
from jax.sharding import PartitionSpec as P


Z, ZLO, Y, X = 8, 4, 8, 4
ROW_GROUPS = [[z * Y + y for y in range(Y)] for z in range(ZLO)]
X_GROUPS = [[2 * x + c for x in range(X)] for c in range(2)]
OTHER_CORE = [(i, i ^ 1) for i in range(2 * X)]
PLANE = ("rep", "fs")
F32, BF16 = jnp.float32, jnp.bfloat16


def z_shift(by):
    return [(z * Y + y, (z + by(z)) % Z * Y + y) for z in range(Z) for y in range(Y)]


def x_shift(by):
    return [(2 * x + c, (x + by(x)) % X * 2 + c) for x in range(X) for c in range(2)]


FROM_NEXT = z_shift(lambda z: -1)
FROM_LAST = z_shift(lambda z: 1)
FROM_TWO = z_shift(lambda z: 2 if z % 2 == 0 else -2)
X_NEXT = x_shift(lambda x: -1)
X_LAST = x_shift(lambda x: 1)
X_TWO = x_shift(lambda x: 2)


def swapped(blocks, axis, groups):
    return lax.all_to_all(blocks, axis, 0, 0, axis_index_groups=groups, tiled=True)


def rolled(a, by, width):
    n = a.shape[1] // width
    out = a
    for k in range(1, n):
        out = jnp.where(by == k, jnp.concatenate([a[:, width * k :], a[:, : width * k]], 1), out)
    return out


VMEM = pl.BlockSpec(memory_space=pltpu.VMEM)
HBM = pl.BlockSpec(memory_space=pltpu.HBM)
SMEM = pl.BlockSpec(memory_space=pltpu.SMEM)


def cost(flops, *arrays):
    return pl.CostEstimate(flops=flops, bytes_accessed=sum(a.size * a.dtype.itemsize for a in arrays), transcendentals=0)


def copies_kernel(*refs):
    *shards, out = refs
    for k, shard in enumerate(shards):
        block = shard[...].astype(out.dtype)
        for i in range(out.shape[0]):
            out[i, k] = block


def copies_of(shards):
    out = jax.ShapeDtypeStruct((Y, len(shards), *shards[0].shape), BF16)
    return pl.pallas_call(
        copies_kernel,
        out_shape=out,
        in_specs=[VMEM] * len(shards),
        out_specs=VMEM,
        compiler_params=pltpu.CompilerParams(vmem_limit_bytes=8 << 20),
        cost_estimate=cost(1 << 28, out, *shards),
        name="copies",
    )(*shards)


def split_kernel(blocks, own, both):
    rows = blocks.shape[2]
    width = own.shape[0]
    for y in range(blocks.shape[0]):
        own[y * rows : (y + 1) * rows] = both[y * rows : (y + 1) * rows] = blocks[y, 0]
        both[width + y * rows : width + (y + 1) * rows] = blocks[y, 1]


def split(blocks):
    count, _, rows, columns = blocks.shape
    own = jax.ShapeDtypeStruct((count * rows, columns), BF16)
    both = jax.ShapeDtypeStruct((2 * count * rows, columns), BF16)
    return pl.pallas_call(
        split_kernel,
        out_shape=[own, both],
        in_specs=[VMEM],
        out_specs=[VMEM] * 2,
        compiler_params=pltpu.CompilerParams(vmem_limit_bytes=8 << 20),
        cost_estimate=cost(1 << 28, own, both, blocks),
        name="split",
    )(blocks)


def by_place_kernel(x_ref, *refs):
    *blocks, out, sems = refs
    rows = blocks[0].shape[0]
    fetches = [
        pltpu.make_async_copy(
            block, out.at[pl.ds(pl.multiple_of((x_ref[0] + k) % X * rows, rows), rows)], sems.at[k]
        )
        for k, block in enumerate(blocks)
    ]
    for fetch in fetches:
        fetch.start()
    for fetch in fetches:
        fetch.wait()


def by_place(x, blocks):
    rows, columns = blocks[0].shape
    return pl.pallas_call(
        by_place_kernel,
        out_shape=jax.ShapeDtypeStruct((X * rows, columns), blocks[0].dtype),
        in_specs=[SMEM] + [HBM] * X,
        out_specs=VMEM,
        scratch_shapes=[pltpu.SemaphoreType.DMA((X,))],
        cost_estimate=cost(1 << 28, *blocks, *blocks),
        compiler_params=pltpu.CompilerParams(vmem_limit_bytes=4 << 20),
        name="by_place",
    )(x[None], *blocks)


def half_kernel(first, a, out):
    out[...] = a[first : first + out.shape[0]]


def half_of(a, part):
    rows = a.shape[0] // 2
    out = jax.ShapeDtypeStruct((rows, a.shape[1]), a.dtype)
    return pl.pallas_call(
        functools.partial(half_kernel, part * rows),
        out_shape=out,
        in_specs=[VMEM],
        out_specs=VMEM,
        cost_estimate=cost(1 << 26, out, out),
        compiler_params=pltpu.CompilerParams(vmem_limit_bytes=1 << 20),
        name="half",
    )(a)


TILE = 256


def fetched(sources, target, sems):
    @pl.when(pl.program_id(0) == 0)
    def _():
        rows = sources[0].shape[0]
        fetches = [
            pltpu.make_async_copy(source, target.at[pl.ds(k * rows, rows)], sems.at[k])
            for k, source in enumerate(sources)
        ]
        for fetch in fetches:
            fetch.start()
        for fetch in fetches:
            fetch.wait()


def early_kernel(half, other, own, u0, u1, u3, early, up, sems):
    fetched((u0, u1, u3), up, sems)
    width, columns = u0.shape

    def write(rows):
        pre = jnp.dot(rows[:, : 2 * width], up[: 2 * width], preferred_element_type=F32)
        pre += jnp.dot(rows[:, 3 * width :], up[2 * width :], preferred_element_type=F32)
        early[:, :columns] = pre.astype(early.dtype)
        early[:, columns:] = rows[:, 2 * width : 3 * width]

    @pl.when(pl.program_id(0) < half)
    def _():
        write(other)

    @pl.when(pl.program_id(0) >= half)
    def _():
        write(own)


def early_of(other, own, blocks):
    rows, d = own.shape
    width, columns = blocks[0].shape
    half = rows // TILE
    shape = (2 * rows, columns + width)
    return pl.pallas_call(
        functools.partial(early_kernel, half),
        grid=(2 * half,),
        out_shape=jax.ShapeDtypeStruct(shape, BF16),
        in_specs=[
            pl.BlockSpec((TILE, d), lambda i: (jnp.minimum(i, half - 1), 0)),
            pl.BlockSpec((TILE, d), lambda i: (jnp.maximum(i - half, 0), 0)),
            *([HBM] * len(blocks)),
        ],
        out_specs=pl.BlockSpec((TILE, shape[1]), lambda i: (i, 0)),
        scratch_shapes=[
            pltpu.VMEM((len(blocks) * width, columns), BF16),
            pltpu.SemaphoreType.DMA((len(blocks),)),
        ],
        compiler_params=pltpu.CompilerParams(vmem_limit_bytes=16 << 20),
        cost_estimate=cost(4 * rows * 3 * width * columns, own, other, *blocks),
        name="early",
    )(other, own, *blocks)


def late_kernel(early, u2_top, u2_bottom, scale, hidden, tiles, up, sems):
    step, steps = pl.program_id(0), early.shape[0] // TILE
    columns = hidden.shape[1]

    def fetch(i):
        rows = pl.ds(i * TILE if isinstance(i, int) else pl.multiple_of(i * TILE, TILE), TILE)
        return pltpu.make_async_copy(early.at[rows], tiles.at[rows], sems.at[i])

    @pl.when(step == 0)
    def _():
        rows = u2_top.shape[0]
        blocks = [
            pltpu.make_async_copy(block, up.at[pl.ds(k * rows, rows)], sems.at[steps + k])
            for k, block in enumerate((u2_top, u2_bottom))
        ]
        for block in blocks:
            block.start()
        for i in range(steps):
            fetch(i).start()
        for block in blocks:
            block.wait()

    fetch(step).wait()
    tile = tiles.at[pl.ds(pl.multiple_of(step * TILE, TILE), TILE)]
    pre = jnp.dot(tile[:, columns:], up[...], preferred_element_type=F32) + tile[:, :columns].astype(F32)
    hidden[...] = jnp.square(jnp.maximum(pre * scale[...], 0.0)).astype(BF16)


def late_of(early, halves, scale):
    width, columns = halves[0].shape
    steps = early.shape[0] // TILE
    out = jax.ShapeDtypeStruct((early.shape[0], columns), BF16)
    return pl.pallas_call(
        late_kernel,
        grid=(steps,),
        out_shape=out,
        in_specs=[HBM, HBM, HBM, pl.BlockSpec((1, columns), lambda i: (0, 0))],
        out_specs=pl.BlockSpec((TILE, columns), lambda i: (i, 0)),
        scratch_shapes=[
            pltpu.VMEM(early.shape, BF16),
            pltpu.VMEM((2 * width, columns), BF16),
            pltpu.SemaphoreType.DMA((steps + 2,)),
        ],
        compiler_params=pltpu.CompilerParams(vmem_limit_bytes=12 << 20),
        cost_estimate=cost(4 * early.shape[0] * width * columns, early, *halves, out),
        name="late",
    )(early, *halves, scale)


def body(tokens, norm_gain, up_weight, up_scale, down_weight, down_scale):
    z = lax.axis_index("fs") // Y
    x = lax.axis_index("tp") // 2
    rows, d = tokens.shape
    width = d // ZLO
    hidden_width = up_weight.shape[1]

    copies = copies_of([up_weight])
    up_own = swapped(copies[:, 0], "fs", ROW_GROUPS).reshape(width, hidden_width)
    down_piece = (down_weight * down_scale).T.astype(BF16)
    down_two = lax.ppermute(down_piece, PLANE, FROM_TWO)

    values = tokens.astype(F32)
    normed = (
        values * lax.rsqrt(jnp.mean(values * values, axis=-1, keepdims=True) + 1e-06) * norm_gain
    ).astype(BF16)
    normed = rolled(normed, z, width)
    near = [
        normed,
        lax.ppermute(normed, "tp", X_NEXT),
        lax.ppermute(normed, "tp", X_TWO),
        lax.ppermute(normed, "tp", X_LAST),
    ]
    own = by_place(x, near)
    other = lax.ppermute(own, "tp", OTHER_CORE)

    up_next = lax.ppermute(up_own, PLANE, FROM_NEXT)
    up_last = lax.ppermute(up_own, PLANE, FROM_LAST)
    up_two = (
        lax.ppermute(half_of(up_next, 0), PLANE, FROM_NEXT),
        lax.ppermute(half_of(up_last, 1), PLANE, FROM_LAST),
    )

    copies = copies_of([down_piece, down_two])
    down_own, down_a = split(swapped(copies, "fs", ROW_GROUPS))
    down_b = jnp.concatenate(
        [lax.ppermute(down_own, PLANE, FROM_NEXT), lax.ppermute(down_own, PLANE, FROM_LAST)], 0
    )
    down_b = lax.optimization_barrier(down_b)

    early = early_of(other, own, (up_own, up_next, up_last))
    hidden = late_of(early, up_two, up_scale)
    hidden_other, hidden_own = hidden[: X * rows], hidden[X * rows :]

    def terms(hidden, down):
        return lax.dot_general(hidden, down, (((1,), (1,)), ((), ())), preferred_element_type=F32)

    def chunk(down, for_other):
        arrived = lax.ppermute(for_other, "tp", OTHER_CORE)
        pair = (terms(hidden_own, down) + arrived.astype(F32)).astype(BF16)
        arrived = swapped(pair.reshape(X, rows, -1), "tp", X_GROUPS)
        return arrived.astype(F32).sum(axis=0).astype(BF16)

    out_a = chunk(down_a, terms(hidden_other, down_a).astype(BF16))
    out_b = chunk(down_b, terms(hidden_other, down_b).astype(BF16))
    summed = jnp.concatenate(
        [out_a[:, :width], out_b[:, :width], out_a[:, width:], out_b[:, width:]], 1
    )
    return rolled(summed, (ZLO - z) % ZLO, width)


def solution(mesh):
    return jax.shard_map(
        body,
        mesh=mesh,
        in_specs=(
            P(("rep", "fs", "tp"), None),
            P(),
            P("fs", "tp"),
            P(None, "tp"),
            P("tp", "fs"),
            P(None, "fs"),
        ),
        out_specs=P(("rep", "fs", "tp"), None),
        check_vma=False,
    )
```

```python
import functools

import jax
import jax.numpy as jnp
from jax import lax
from jax.experimental import pallas as pl
from jax.experimental.pallas import tpu as pltpu
from jax.sharding import PartitionSpec as P


Z, ZLO, Y, X = 8, 4, 8, 4
ROW_GROUPS = [[z * Y + y for y in range(Y)] for z in range(ZLO)]
X_GROUPS = [[2 * x + c for x in range(X)] for c in range(2)]
OTHER_CORE = [(i, i ^ 1) for i in range(2 * X)]
PLANE = ("rep", "fs")
F32, BF16 = jnp.float32, jnp.bfloat16


def z_shift(by):
    return [(z * Y + y, (z + by(z)) % Z * Y + y) for z in range(Z) for y in range(Y)]


def x_shift(by):
    return [(2 * x + c, (x + by(x)) % X * 2 + c) for x in range(X) for c in range(2)]


FROM_NEXT = z_shift(lambda z: -1)
FROM_LAST = z_shift(lambda z: 1)
FROM_TWO = z_shift(lambda z: 2 if z % 2 == 0 else -2)
X_NEXT = x_shift(lambda x: -1)
X_LAST = x_shift(lambda x: 1)
X_TWO = x_shift(lambda x: 2)


def swapped(blocks, axis, groups):
    return lax.all_to_all(blocks, axis, 0, 0, axis_index_groups=groups, tiled=True)


def rolled(a, by, width):
    n = a.shape[1] // width
    out = a
    for k in range(1, n):
        out = jnp.where(by == k, jnp.concatenate([a[:, width * k :], a[:, : width * k]], 1), out)
    return out


VMEM = pl.BlockSpec(memory_space=pltpu.VMEM)
HBM = pl.BlockSpec(memory_space=pltpu.HBM)
SMEM = pl.BlockSpec(memory_space=pltpu.SMEM)


def cost(flops, *arrays):
    return pl.CostEstimate(flops=flops, bytes_accessed=sum(a.size * a.dtype.itemsize for a in arrays), transcendentals=0)


def copies_kernel(*refs):
    *shards, out = refs
    for k, shard in enumerate(shards):
        block = shard[...].astype(out.dtype)
        for i in range(out.shape[0]):
            out[i, k] = block


def copies_of(shards):
    out = jax.ShapeDtypeStruct((Y, len(shards), *shards[0].shape), BF16)
    return pl.pallas_call(
        copies_kernel,
        out_shape=out,
        in_specs=[VMEM] * len(shards),
        out_specs=VMEM,
        compiler_params=pltpu.CompilerParams(vmem_limit_bytes=8 << 20),
        cost_estimate=cost(1 << 28, out, *shards),
        name="copies",
    )(*shards)


def split_kernel(blocks, own, both):
    rows = blocks.shape[2]
    width = own.shape[0]
    for y in range(blocks.shape[0]):
        own[y * rows : (y + 1) * rows] = both[y * rows : (y + 1) * rows] = blocks[y, 0]
        both[width + y * rows : width + (y + 1) * rows] = blocks[y, 1]


def split(blocks):
    count, _, rows, columns = blocks.shape
    own = jax.ShapeDtypeStruct((count * rows, columns), BF16)
    both = jax.ShapeDtypeStruct((2 * count * rows, columns), BF16)
    return pl.pallas_call(
        split_kernel,
        out_shape=[own, both],
        in_specs=[VMEM],
        out_specs=[VMEM] * 2,
        compiler_params=pltpu.CompilerParams(vmem_limit_bytes=8 << 20),
        cost_estimate=cost(1 << 28, own, both, blocks),
        name="split",
    )(blocks)


def by_place_kernel(x_ref, *refs):
    *blocks, out, sems = refs
    rows = blocks[0].shape[0]
    fetches = [
        pltpu.make_async_copy(
            block, out.at[pl.ds(pl.multiple_of((x_ref[0] + k) % X * rows, rows), rows)], sems.at[k]
        )
        for k, block in enumerate(blocks)
    ]
    for fetch in fetches:
        fetch.start()
    for fetch in fetches:
        fetch.wait()


def by_place(x, blocks):
    rows, columns = blocks[0].shape
    return pl.pallas_call(
        by_place_kernel,
        out_shape=jax.ShapeDtypeStruct((X * rows, columns), blocks[0].dtype),
        in_specs=[SMEM] + [HBM] * X,
        out_specs=VMEM,
        scratch_shapes=[pltpu.SemaphoreType.DMA((X,))],
        cost_estimate=cost(1 << 28, *blocks, *blocks),
        compiler_params=pltpu.CompilerParams(vmem_limit_bytes=4 << 20),
        name="by_place",
    )(x[None], *blocks)


def half_kernel(first, a, out):
    out[...] = a[first : first + out.shape[0]]


def half_of(a, part):
    rows = a.shape[0] // 2
    out = jax.ShapeDtypeStruct((rows, a.shape[1]), a.dtype)
    return pl.pallas_call(
        functools.partial(half_kernel, part * rows),
        out_shape=out,
        in_specs=[VMEM],
        out_specs=VMEM,
        cost_estimate=cost(1 << 26, out, out),
        compiler_params=pltpu.CompilerParams(vmem_limit_bytes=1 << 20),
        name="half",
    )(a)


def stacked_kernel(*refs):
    *blocks, out, sems = refs
    rows = blocks[0].shape[0]
    fetches = [
        pltpu.make_async_copy(block, out.at[pl.ds(k * rows, rows)], sems.at[k]) for k, block in enumerate(blocks)
    ]
    for fetch in fetches:
        fetch.start()
    for fetch in fetches:
        fetch.wait()


def stacked(blocks):
    rows, columns = blocks[0].shape
    return pl.pallas_call(
        stacked_kernel,
        out_shape=jax.ShapeDtypeStruct((len(blocks) * rows, columns), blocks[0].dtype),
        in_specs=[HBM] * len(blocks),
        out_specs=VMEM,
        scratch_shapes=[pltpu.SemaphoreType.DMA((len(blocks),))],
        cost_estimate=cost(1 << 28, *blocks, *blocks),
        compiler_params=pltpu.CompilerParams(vmem_limit_bytes=4 << 20),
        name="stacked",
    )(*blocks)


TILE = 256


def fetched(sources, target, sems):
    @pl.when(pl.program_id(0) == 0)
    def _():
        rows = sources[0].shape[0]
        fetches = [
            pltpu.make_async_copy(source, target.at[pl.ds(k * rows, rows)], sems.at[k])
            for k, source in enumerate(sources)
        ]
        for fetch in fetches:
            fetch.start()
        for fetch in fetches:
            fetch.wait()


def early_kernel(half, other, own, u0, u1, u3, early, up, sems):
    fetched((u0, u1, u3), up, sems)
    width, columns = u0.shape

    def write(rows):
        pre = jnp.dot(rows[:, : 2 * width], up[: 2 * width], preferred_element_type=F32)
        pre += jnp.dot(rows[:, 3 * width :], up[2 * width :], preferred_element_type=F32)
        early[:, :columns] = pre.astype(early.dtype)
        early[:, columns:] = rows[:, 2 * width : 3 * width]

    @pl.when(pl.program_id(0) < half)
    def _():
        write(other)

    @pl.when(pl.program_id(0) >= half)
    def _():
        write(own)


def early_of(other, own, blocks):
    rows, d = own.shape
    width, columns = blocks[0].shape
    half = rows // TILE
    shape = (2 * rows, columns + width)
    return pl.pallas_call(
        functools.partial(early_kernel, half),
        grid=(2 * half,),
        out_shape=jax.ShapeDtypeStruct(shape, BF16),
        in_specs=[
            pl.BlockSpec((TILE, d), lambda i: (jnp.minimum(i, half - 1), 0)),
            pl.BlockSpec((TILE, d), lambda i: (jnp.maximum(i - half, 0), 0)),
            *([HBM] * len(blocks)),
        ],
        out_specs=pl.BlockSpec((TILE, shape[1]), lambda i: (i, 0)),
        scratch_shapes=[
            pltpu.VMEM((len(blocks) * width, columns), BF16),
            pltpu.SemaphoreType.DMA((len(blocks),)),
        ],
        compiler_params=pltpu.CompilerParams(vmem_limit_bytes=16 << 20),
        cost_estimate=cost(4 * rows * 3 * width * columns, own, other, *blocks),
        name="early",
    )(other, own, *blocks)


def late_kernel(early, u2_top, u2_bottom, scale, hidden, tiles, up, sems):
    step, steps = pl.program_id(0), early.shape[0] // TILE
    columns = hidden.shape[1]

    def fetch(i):
        rows = pl.ds(i * TILE if isinstance(i, int) else pl.multiple_of(i * TILE, TILE), TILE)
        return pltpu.make_async_copy(early.at[rows], tiles.at[rows], sems.at[i])

    @pl.when(step == 0)
    def _():
        rows = u2_top.shape[0]
        blocks = [
            pltpu.make_async_copy(block, up.at[pl.ds(k * rows, rows)], sems.at[steps + k])
            for k, block in enumerate((u2_top, u2_bottom))
        ]
        for block in blocks:
            block.start()
        for i in range(steps):
            fetch(i).start()
        for block in blocks:
            block.wait()

    fetch(step).wait()
    tile = tiles.at[pl.ds(pl.multiple_of(step * TILE, TILE), TILE)]
    pre = jnp.dot(tile[:, columns:], up[...], preferred_element_type=F32) + tile[:, :columns].astype(F32)
    hidden[...] = jnp.square(jnp.maximum(pre * scale[...], 0.0)).astype(BF16)


def late_of(early, halves, scale):
    width, columns = halves[0].shape
    steps = early.shape[0] // TILE
    out = jax.ShapeDtypeStruct((early.shape[0], columns), BF16)
    return pl.pallas_call(
        late_kernel,
        grid=(steps,),
        out_shape=out,
        in_specs=[HBM, HBM, HBM, pl.BlockSpec((1, columns), lambda i: (0, 0))],
        out_specs=pl.BlockSpec((TILE, columns), lambda i: (i, 0)),
        scratch_shapes=[
            pltpu.VMEM(early.shape, BF16),
            pltpu.VMEM((2 * width, columns), BF16),
            pltpu.SemaphoreType.DMA((steps + 2,)),
        ],
        compiler_params=pltpu.CompilerParams(vmem_limit_bytes=12 << 20),
        cost_estimate=cost(4 * early.shape[0] * width * columns, early, *halves, out),
        name="late",
    )(early, *halves, scale)


def body(tokens, norm_gain, up_weight, up_scale, down_weight, down_scale):
    z = lax.axis_index("fs") // Y
    x = lax.axis_index("tp") // 2
    rows, d = tokens.shape
    width = d // ZLO
    hidden_width = up_weight.shape[1]

    copies = copies_of([up_weight])
    up_own = swapped(copies[:, 0], "fs", ROW_GROUPS).reshape(width, hidden_width)
    down_piece = (down_weight * down_scale).T.astype(BF16)
    down_two = lax.ppermute(down_piece, PLANE, FROM_TWO)

    values = tokens.astype(F32)
    normed = (
        values * lax.rsqrt(jnp.mean(values * values, axis=-1, keepdims=True) + 1e-06) * norm_gain
    ).astype(BF16)
    normed = rolled(normed, z, width)
    near = [
        normed,
        lax.ppermute(normed, "tp", X_NEXT),
        lax.ppermute(normed, "tp", X_TWO),
        lax.ppermute(normed, "tp", X_LAST),
    ]
    own = by_place(x, near)
    other = lax.ppermute(own, "tp", OTHER_CORE)

    up_next = lax.ppermute(up_own, PLANE, FROM_NEXT)
    up_last = lax.ppermute(up_own, PLANE, FROM_LAST)
    up_two = (
        lax.ppermute(half_of(up_next, 0), PLANE, FROM_NEXT),
        lax.ppermute(half_of(up_last, 1), PLANE, FROM_LAST),
    )

    copies = copies_of([down_piece, down_two])
    down_own, down_a = split(swapped(copies, "fs", ROW_GROUPS))
    down_b = stacked(
        [lax.ppermute(down_own, PLANE, FROM_NEXT), lax.ppermute(down_own, PLANE, FROM_LAST)]
    )

    early = early_of(other, own, (up_own, up_next, up_last))
    hidden = late_of(early, up_two, up_scale)
    hidden_other, hidden_own = hidden[: X * rows], hidden[X * rows :]

    def terms(hidden, down):
        return lax.dot_general(hidden, down, (((1,), (1,)), ((), ())), preferred_element_type=F32)

    def chunk(down, for_other):
        arrived = lax.ppermute(for_other, "tp", OTHER_CORE)
        mine = lax.optimization_barrier(terms(hidden_own, down))
        pair = (mine + arrived.astype(F32)).astype(BF16)
        arrived = swapped(pair.reshape(X, rows, -1), "tp", X_GROUPS)
        return arrived.astype(F32).sum(axis=0).astype(BF16)

    out_a = chunk(down_a, terms(hidden_other, down_a).astype(BF16))
    out_b = chunk(down_b, terms(hidden_other, down_b).astype(BF16))
    summed = jnp.concatenate(
        [out_a[:, :width], out_b[:, :width], out_a[:, width:], out_b[:, width:]], 1
    )
    return rolled(summed, (ZLO - z) % ZLO, width)


def solution(mesh):
    return jax.shard_map(
        body,
        mesh=mesh,
        in_specs=(
            P(("rep", "fs", "tp"), None),
            P(),
            P("fs", "tp"),
            P(None, "tp"),
            P("tp", "fs"),
            P(None, "fs"),
        ),
        out_specs=P(("rep", "fs", "tp"), None),
        check_vma=False,
    )
```

```python
import functools

import jax
import jax.numpy as jnp
from jax import lax
from jax.experimental import pallas as pl
from jax.experimental.pallas import tpu as pltpu
from jax.sharding import PartitionSpec as P


Z, ZLO, Y, X = 8, 4, 8, 4
ROW_GROUPS = [[z * Y + y for y in range(Y)] for z in range(ZLO)]
X_GROUPS = [[2 * x + c for x in range(X)] for c in range(2)]
OTHER_CORE = [(i, i ^ 1) for i in range(2 * X)]
PLANE = ("rep", "fs")
F32, BF16 = jnp.float32, jnp.bfloat16


def z_shift(by):
    return [(z * Y + y, (z + by(z)) % Z * Y + y) for z in range(Z) for y in range(Y)]


def x_shift(by):
    return [(2 * x + c, (x + by(x)) % X * 2 + c) for x in range(X) for c in range(2)]


FROM_NEXT = z_shift(lambda z: -1)
FROM_LAST = z_shift(lambda z: 1)
FROM_TWO = z_shift(lambda z: 2 if z % 2 == 0 else -2)
X_NEXT = x_shift(lambda x: -1)
X_LAST = x_shift(lambda x: 1)
X_TWO = x_shift(lambda x: 2)


def swapped(blocks, axis, groups):
    return lax.all_to_all(blocks, axis, 0, 0, axis_index_groups=groups, tiled=True)


def rolled(a, by, width):
    n = a.shape[1] // width
    out = a
    for k in range(1, n):
        out = jnp.where(by == k, jnp.concatenate([a[:, width * k :], a[:, : width * k]], 1), out)
    return out


VMEM = pl.BlockSpec(memory_space=pltpu.VMEM)
HBM = pl.BlockSpec(memory_space=pltpu.HBM)
SMEM = pl.BlockSpec(memory_space=pltpu.SMEM)


def cost(flops, *arrays):
    return pl.CostEstimate(flops=flops, bytes_accessed=sum(a.size * a.dtype.itemsize for a in arrays), transcendentals=0)


def copies_kernel(*refs):
    *shards, out = refs
    for k, shard in enumerate(shards):
        block = shard[...].astype(out.dtype)
        for i in range(out.shape[0]):
            out[i, k] = block


def copies_of(shards):
    out = jax.ShapeDtypeStruct((Y, len(shards), *shards[0].shape), BF16)
    return pl.pallas_call(
        copies_kernel,
        out_shape=out,
        in_specs=[VMEM] * len(shards),
        out_specs=VMEM,
        compiler_params=pltpu.CompilerParams(vmem_limit_bytes=8 << 20),
        cost_estimate=cost(1 << 28, out, *shards),
        name="copies",
    )(*shards)


def split_kernel(blocks, own, both):
    rows = blocks.shape[2]
    width = own.shape[0]
    for y in range(blocks.shape[0]):
        own[y * rows : (y + 1) * rows] = both[y * rows : (y + 1) * rows] = blocks[y, 0]
        both[width + y * rows : width + (y + 1) * rows] = blocks[y, 1]


def split(blocks):
    count, _, rows, columns = blocks.shape
    own = jax.ShapeDtypeStruct((count * rows, columns), BF16)
    both = jax.ShapeDtypeStruct((2 * count * rows, columns), BF16)
    return pl.pallas_call(
        split_kernel,
        out_shape=[own, both],
        in_specs=[VMEM],
        out_specs=[VMEM] * 2,
        compiler_params=pltpu.CompilerParams(vmem_limit_bytes=8 << 20),
        cost_estimate=cost(1 << 28, own, both, blocks),
        name="split",
    )(blocks)


def by_place_kernel(x_ref, *refs):
    *blocks, out, sems = refs
    rows = blocks[0].shape[0]
    fetches = [
        pltpu.make_async_copy(
            block, out.at[pl.ds(pl.multiple_of((x_ref[0] + k) % X * rows, rows), rows)], sems.at[k]
        )
        for k, block in enumerate(blocks)
    ]
    for fetch in fetches:
        fetch.start()
    for fetch in fetches:
        fetch.wait()


def by_place(x, blocks):
    rows, columns = blocks[0].shape
    return pl.pallas_call(
        by_place_kernel,
        out_shape=jax.ShapeDtypeStruct((X * rows, columns), blocks[0].dtype),
        in_specs=[SMEM] + [HBM] * X,
        out_specs=VMEM,
        scratch_shapes=[pltpu.SemaphoreType.DMA((X,))],
        cost_estimate=cost(1 << 28, *blocks, *blocks),
        compiler_params=pltpu.CompilerParams(vmem_limit_bytes=4 << 20),
        name="by_place",
    )(x[None], *blocks)


def half_kernel(first, a, out):
    out[...] = a[first : first + out.shape[0]]


def half_of(a, part):
    rows = a.shape[0] // 2
    out = jax.ShapeDtypeStruct((rows, a.shape[1]), a.dtype)
    return pl.pallas_call(
        functools.partial(half_kernel, part * rows),
        out_shape=out,
        in_specs=[VMEM],
        out_specs=VMEM,
        cost_estimate=cost(1 << 26, out, out),
        compiler_params=pltpu.CompilerParams(vmem_limit_bytes=1 << 20),
        name="half",
    )(a)


def stacked_kernel(*refs):
    *blocks, out, sems = refs
    rows = blocks[0].shape[0]
    fetches = [
        pltpu.make_async_copy(block, out.at[pl.ds(k * rows, rows)], sems.at[k]) for k, block in enumerate(blocks)
    ]
    for fetch in fetches:
        fetch.start()
    for fetch in fetches:
        fetch.wait()


def stacked(blocks):
    rows, columns = blocks[0].shape
    return pl.pallas_call(
        stacked_kernel,
        out_shape=jax.ShapeDtypeStruct((len(blocks) * rows, columns), blocks[0].dtype),
        in_specs=[HBM] * len(blocks),
        out_specs=VMEM,
        scratch_shapes=[pltpu.SemaphoreType.DMA((len(blocks),))],
        cost_estimate=cost(1 << 28, *blocks, *blocks),
        compiler_params=pltpu.CompilerParams(vmem_limit_bytes=4 << 20),
        name="stacked",
    )(*blocks)


TILE = 512


def fetched(sources, target, sems):
    @pl.when(pl.program_id(0) == 0)
    def _():
        rows = sources[0].shape[0]
        fetches = [
            pltpu.make_async_copy(source, target.at[pl.ds(k * rows, rows)], sems.at[k])
            for k, source in enumerate(sources)
        ]
        for fetch in fetches:
            fetch.start()
        for fetch in fetches:
            fetch.wait()


def early_kernel(half, other, own, u0, u1, u3, early, up, sems):
    fetched((u0, u1, u3), up, sems)
    width, columns = u0.shape

    def write(rows):
        pre = jnp.dot(rows[:, : 2 * width], up[: 2 * width], preferred_element_type=F32)
        pre += jnp.dot(rows[:, 3 * width :], up[2 * width :], preferred_element_type=F32)
        early[:, :columns] = pre.astype(early.dtype)
        early[:, columns:] = rows[:, 2 * width : 3 * width]

    @pl.when(pl.program_id(0) < half)
    def _():
        write(other)

    @pl.when(pl.program_id(0) >= half)
    def _():
        write(own)


def early_of(other, own, blocks):
    rows, d = own.shape
    width, columns = blocks[0].shape
    half = rows // TILE
    shape = (2 * rows, columns + width)
    return pl.pallas_call(
        functools.partial(early_kernel, half),
        grid=(2 * half,),
        out_shape=pltpu.HBM(shape, BF16),
        in_specs=[
            pl.BlockSpec((TILE, d), lambda i: (jnp.minimum(i, half - 1), 0)),
            pl.BlockSpec((TILE, d), lambda i: (jnp.maximum(i - half, 0), 0)),
            *([HBM] * len(blocks)),
        ],
        out_specs=pl.BlockSpec((TILE, shape[1]), lambda i: (i, 0)),
        scratch_shapes=[
            pltpu.VMEM((len(blocks) * width, columns), BF16),
            pltpu.SemaphoreType.DMA((len(blocks),)),
        ],
        compiler_params=pltpu.CompilerParams(vmem_limit_bytes=16 << 20),
        cost_estimate=cost(4 * rows * 3 * width * columns, own, other, *blocks),
        name="early",
    )(other, own, *blocks)


def late_kernel(early, u2_top, u2_bottom, scale, hidden, tiles, up, sems):
    step, steps = pl.program_id(0), early.shape[0] // TILE
    columns = hidden.shape[1]

    def fetch(i):
        rows = pl.ds(i * TILE if isinstance(i, int) else pl.multiple_of(i * TILE, TILE), TILE)
        return pltpu.make_async_copy(early.at[rows], tiles.at[rows], sems.at[i])

    @pl.when(step == 0)
    def _():
        rows = u2_top.shape[0]
        blocks = [
            pltpu.make_async_copy(block, up.at[pl.ds(k * rows, rows)], sems.at[steps + k])
            for k, block in enumerate((u2_top, u2_bottom))
        ]
        for block in blocks:
            block.start()
        for i in range(steps):
            fetch(i).start()
        for block in blocks:
            block.wait()

    fetch(step).wait()
    tile = tiles.at[pl.ds(pl.multiple_of(step * TILE, TILE), TILE)]
    pre = jnp.dot(tile[:, columns:], up[...], preferred_element_type=F32) + tile[:, :columns].astype(F32)
    hidden[...] = jnp.square(jnp.maximum(pre * scale[...], 0.0)).astype(BF16)


def late_of(early, halves, scale):
    width, columns = halves[0].shape
    steps = early.shape[0] // TILE
    out = jax.ShapeDtypeStruct((early.shape[0], columns), BF16)
    return pl.pallas_call(
        late_kernel,
        grid=(steps,),
        out_shape=out,
        in_specs=[HBM, HBM, HBM, pl.BlockSpec((1, columns), lambda i: (0, 0))],
        out_specs=pl.BlockSpec((TILE, columns), lambda i: (i, 0)),
        scratch_shapes=[
            pltpu.VMEM(early.shape, BF16),
            pltpu.VMEM((2 * width, columns), BF16),
            pltpu.SemaphoreType.DMA((steps + 2,)),
        ],
        compiler_params=pltpu.CompilerParams(vmem_limit_bytes=12 << 20),
        cost_estimate=cost(4 * early.shape[0] * width * columns, early, *halves, out),
        name="late",
    )(pltpu.with_memory_space_constraint(early, pltpu.HBM), *halves, scale)


def body(tokens, norm_gain, up_weight, up_scale, down_weight, down_scale):
    z = lax.axis_index("fs") // Y
    x = lax.axis_index("tp") // 2
    rows, d = tokens.shape
    width = d // ZLO
    hidden_width = up_weight.shape[1]

    copies = copies_of([up_weight])
    up_own = swapped(copies[:, 0], "fs", ROW_GROUPS).reshape(width, hidden_width)
    down_piece = (down_weight * down_scale).T.astype(BF16)
    down_two = lax.ppermute(down_piece, PLANE, FROM_TWO)

    values = tokens.astype(F32)
    normed = (
        values * lax.rsqrt(jnp.mean(values * values, axis=-1, keepdims=True) + 1e-06) * norm_gain
    ).astype(BF16)
    normed = rolled(normed, z, width)
    near = [
        normed,
        lax.ppermute(normed, "tp", X_NEXT),
        lax.ppermute(normed, "tp", X_TWO),
        lax.ppermute(normed, "tp", X_LAST),
    ]
    own = by_place(x, near)
    other = lax.ppermute(own, "tp", OTHER_CORE)

    up_next = lax.ppermute(up_own, PLANE, FROM_NEXT)
    up_last = lax.ppermute(up_own, PLANE, FROM_LAST)
    up_two = (
        lax.ppermute(half_of(up_next, 0), PLANE, FROM_NEXT),
        lax.ppermute(half_of(up_last, 1), PLANE, FROM_LAST),
    )

    copies = copies_of([down_piece, down_two])
    down_own, down_a = split(swapped(copies, "fs", ROW_GROUPS))
    down_b = stacked(
        [lax.ppermute(down_own, PLANE, FROM_NEXT), lax.ppermute(down_own, PLANE, FROM_LAST)]
    )

    early = early_of(other, own, (up_own, up_next, up_last))
    hidden = late_of(early, up_two, up_scale)
    hidden_other, hidden_own = hidden[: X * rows], hidden[X * rows :]

    def terms(hidden, down):
        return lax.dot_general(hidden, down, (((1,), (1,)), ((), ())), preferred_element_type=F32)

    def chunk(down, for_other):
        arrived = lax.ppermute(for_other, "tp", OTHER_CORE)
        mine = lax.optimization_barrier(terms(hidden_own, down))
        pair = (mine + arrived.astype(F32)).astype(BF16)
        arrived = swapped(pair.reshape(X, rows, -1), "tp", X_GROUPS)
        return arrived.astype(F32).sum(axis=0).astype(BF16)

    out_a = chunk(down_a, terms(hidden_other, down_a).astype(BF16))
    out_b = chunk(down_b, terms(hidden_other, down_b).astype(BF16))
    summed = jnp.concatenate(
        [out_a[:, :width], out_b[:, :width], out_a[:, width:], out_b[:, width:]], 1
    )
    return rolled(summed, (ZLO - z) % ZLO, width)


def solution(mesh):
    return jax.shard_map(
        body,
        mesh=mesh,
        in_specs=(
            P(("rep", "fs", "tp"), None),
            P(),
            P("fs", "tp"),
            P(None, "tp"),
            P("tp", "fs"),
            P(None, "fs"),
        ),
        out_specs=P(("rep", "fs", "tp"), None),
        check_vma=False,
    )
```
